32 devices in a mesh: ep: 16 (over z, y, core), tp: 2 (over x).
Axes of the slice: x: 2, y: 2, z: 4, core: 2. Of those that a mesh axis runs over, the one named last changes fastest.
Arguments:
- resid: bfloat16 [256, 2048], P('ep'), may hold values from -40 to 40
- queries: bfloat16 [256, 1024], P('ep', 'tp'), may hold values from -146 to 146
- new_keys: bfloat16 [256, 512], P('ep', 'tp'), may hold values from -6 to 6
- new_values: bfloat16 [256, 512], P('ep', 'tp'), may hold values from -18 to 18
- key_cache: bfloat16 [256, 4, 256, 128], P('ep', 'tp'), may hold values from -5 to 5
- value_cache: bfloat16 [256, 4, 256, 128], P('ep', 'tp'), may hold values from -18 to 18
- cum_gate: float32 [256, 8, 256], P('ep', 'tp'), may hold values from -256 to 0, as said below
- forget_logit: float32 [256, 8], P('ep', 'tp'), may hold values from -6 to 6
- forget_bias: float32 [8], P('tp'), may hold values from -3 to 2
- lengths: int32 [256], P('ep'), may hold values from 32 to 256
- out_weight: bfloat16 [1024, 2048], P('tp'), may hold values from -0.1875 to 0.1875
- norm_gain: float32 [2048], replicated, may hold values from 0.1 to 1.9
- mix_vector: bfloat16 [2048], replicated, may hold values from -0.125 to 0.125
- routes: int32 [256, 2], P('ep'), may hold values from 0 to 3, all different within a row; in each aligned block of 16 rows (0 to 15, 16 to 31, ...) at most 16 rows name the same one
- route_weight: float32 [256, 2], P('ep'), may hold values from 0.2 to 1
- expert_gate: bfloat16 [16, 2048, 768], P('ep', 'tp'), may hold values from -0.125 to 0.125
- expert_up: bfloat16 [16, 2048, 768], P('ep', 'tp'), may hold values from -0.125 to 0.125
- expert_down: bfloat16 [16, 768, 2048], P('ep', None, 'tp'), may hold values from -0.109375 to 0.109375
- dense_gate: bfloat16 [2048, 3072], P('tp', 'ep'), may hold values from -0.125 to 0.125
- dense_up: bfloat16 [2048, 3072], P('tp', 'ep'), may hold values from -0.125 to 0.125
- dense_down: bfloat16 [3072, 2048], P('ep', 'tp'), may hold values from -0.109375 to 0.109375
Outputs:
- layer_out: bfloat16 [256, 2048], P('ep', 'tp')
The draws below stay inside these ranges and needn't reach their ends.
Inputs may be any that keep to these rules, and one draw needn't show every extreme that they name: `routes`: each row names 2 different experts; the rows of one index of ep name no expert more than 16 times. `cum_gate`: for positions below the sequence's length, the running sum of the log forget gates of positions 0 to p; it never rises along p.
All inputs are finite; a program needn't handle non-finite values.
Results may differ from the reference program's by a relative error of at most 0.0095.
Values may be sent and summed in bfloat16 or wider, within the bound.
No kernel may reach another device: no remote copies, remote signals or barrier semaphores. Data moves between devices by JAX's collectives and lax.ppermute only.
A program may use at most 64 MiB of HBM per device.

```python
import math
import jax
import jax.numpy as jnp
import numpy as np
from jax import lax

D = 2048
QUERY_HEADS = 8
KV_HEADS = 4
HEAD = 128
FF = 3072
FFD = 3072
TOP_K = 2
EXP_SPAN = 4
SEQ_DEV = 16
CACHE_SLOTS = 256
SEQUENCE_TOTAL = 256
EXPERTS = 4
CAP = 16
FF_SPAN = 768
N_EP = 16
N_TP = 2


def first_keys(key):
    return jnp.clip(jax.random.normal(jax.random.fold_in(key, 11), (SEQUENCE_TOTAL, KV_HEADS, HEAD), jnp.float32), -5.0, 5.0)


def draw_key_cache(key, part):
    leading = first_keys(key)
    others = jnp.clip(jax.random.normal(jax.random.fold_in(key, 12), (SEQUENCE_TOTAL, KV_HEADS, CACHE_SLOTS, HEAD), jnp.float32), -5.0, 5.0)
    full = others.at[:, :, 0, :].set(leading)
    return full.astype(jnp.bfloat16)


def draw_queries(key, part):
    base = jnp.clip(jax.random.normal(jax.random.fold_in(key, 15), (SEQUENCE_TOTAL, QUERY_HEADS, HEAD), jnp.float32), -5.0, 5.0)
    return base.reshape(SEQUENCE_TOTAL, QUERY_HEADS * HEAD).astype(jnp.bfloat16)


def draw_resid(key, part):
    block_index = jnp.arange(D) * N_TP // D
    rising = 3.0 ** (block_index.astype(jnp.float32) / max(N_TP - 1, 1))
    column = jnp.exp(jax.random.uniform(jax.random.fold_in(key, 21), (D,), jnp.float32, 0.0, math.log(3.0)))
    base = jnp.clip(jax.random.normal(jax.random.fold_in(key, 22), (SEQUENCE_TOTAL, D), jnp.float32), -4.0, 4.0)
    rowscale = jnp.exp(jax.random.uniform(jax.random.fold_in(key, 23), (SEQUENCE_TOTAL,), jnp.float32, math.log(0.3), math.log(3.0)))
    values = base * rowscale[:, None] * (column * rising)[None, :] / 3.0
    return jnp.clip(values, -40.0, 40.0).astype(jnp.bfloat16)


def draw_cum_gate(key, part):
    slow_share = 0.5
    slower_path = jax.random.uniform(jax.random.fold_in(key, 31), (SEQUENCE_TOTAL, QUERY_HEADS, 1), jnp.float32) < slow_share
    whole_loss = jnp.exp(jax.random.uniform(jax.random.fold_in(key, 32), (SEQUENCE_TOTAL, QUERY_HEADS, 1), jnp.float32, math.log(0.5), math.log(2.0)))
    fast_rate = jnp.exp(jax.random.uniform(jax.random.fold_in(key, 33), (SEQUENCE_TOTAL, QUERY_HEADS, 1), jnp.float32, math.log(0.01), math.log(1.0 / 30.0)))
    decay_rate = jnp.where(slower_path, whole_loss / CACHE_SLOTS, fast_rate)
    coarse_estimate = jax.random.uniform(jax.random.fold_in(key, 34), (SEQUENCE_TOTAL, QUERY_HEADS, CACHE_SLOTS), jnp.float32, 0.2, 1.8)
    quarter = jnp.exp(jax.random.uniform(jax.random.fold_in(key, 35), (SEQUENCE_TOTAL, QUERY_HEADS, 4), jnp.float32, math.log(0.5), math.log(2.0)))
    per_block_pass = jnp.repeat(quarter, CACHE_SLOTS // 4, axis=2)
    sudden_spike = jax.random.uniform(jax.random.fold_in(key, 36), (SEQUENCE_TOTAL, QUERY_HEADS, CACHE_SLOTS), jnp.float32) < 3.0 / CACHE_SLOTS
    dropped_amount = jnp.log(jax.random.uniform(jax.random.fold_in(key, 37), (SEQUENCE_TOTAL, QUERY_HEADS, CACHE_SLOTS), jnp.float32, 0.5, 0.8))
    decode_steps = -decay_rate * coarse_estimate * per_block_pass + jnp.where(sudden_spike & slower_path, dropped_amount, 0.0)
    return jnp.cumsum(decode_steps, axis=2).astype(jnp.float32)


def touch_ends(values, key, low, high):
    longest = values.shape.index(max(values.shape))
    spots = []
    for shift in (0, 1):
        where = [jax.random.randint(jax.random.fold_in(key, axis), (), 0, length) for axis, length in enumerate(values.shape)]
        where[longest] = (where[longest] + shift) % values.shape[longest]
        spots.append(tuple(where))
    return values.at[spots[0]].set(low).at[spots[1]].set(high)


def steps_of(key, dims, cuts, smallest, high):
    def one(dim, shards_of):
        draws = jax.random.uniform(jax.random.fold_in(jax.random.fold_in(key, 6), dim), (shards_of,), jnp.float32, smallest / len(cuts), high / len(cuts))
        return jnp.repeat(jnp.exp(draws), dims[dim] // shards_of).reshape((-1,) + (1,) * (len(dims) - dim - 1))

    level = one(*cuts[0])
    for cut in cuts[1:]:
        level = level * one(*cut)
    return level


def shared_out(key, own, number, rows, number_of, top, most, lean):
    sequence = jax.random.permutation(key, number_of)
    crowded, usual = load_shares(number_of, rows * top, most, lean, True), load_shares(number_of, rows * top, most, lean, False)
    places = jnp.arange(number_of)

    def named(tallies, rotation):
        used = int((tallies > 0).sum())
        fixed = max(1, used // 4)
        moved = fixed + (places - fixed + rotation * (used - fixed)) % max(1, number_of - fixed)
        return jnp.zeros((number_of,), jnp.int32).at[sequence[jnp.where(places < fixed, places, moved)]].set(jnp.asarray(tallies, jnp.int32))

    tallies = jnp.where(number % 4 == 0, named(crowded, number // 4), named(usual, number - number // 4 - 1))
    mixed = jax.random.permutation(jax.random.fold_in(own, 3), number_of)
    giver, taker = mixed[0:number_of // 2 * 2:2], mixed[1:number_of // 2 * 2:2]
    slack = jnp.minimum(tallies[giver] - 1, most - tallies[taker]) // 2
    slack = jnp.where((giver == sequence[0]) | (taker == sequence[0]) | (tallies[taker] == 0), 0, jnp.maximum(slack, 0))
    moved = jax.random.randint(jax.random.fold_in(own, 4), (number_of // 2,), 0, 1 << 20) % (slack + 1)
    tallies = tallies.at[giver].add(-moved).at[taker].add(moved)
    labels = jnp.searchsorted(jnp.cumsum(tallies), jnp.arange(rows * top), side="right").astype(jnp.int32)
    listing = labels.reshape(top, rows).T
    listing = listing[jax.random.permutation(jax.random.fold_in(own, 1), rows)]
    rotation = jax.random.randint(jax.random.fold_in(own, 2), (rows, 1), 0, top)
    return jnp.take_along_axis(listing, (jnp.arange(top)[None, :] + rotation) % top, axis=1)


def load_shares(amount, total, reach, skew, full):
    loads = [(1 << 20) // math.isqrt(rank ** skew) + 1 for rank in range(1, amount + 1)]
    largest = reach if full else min(reach, max(-(-total // amount), total * loads[0] // sum(loads)))
    least = 1 if total - largest >= amount - 1 else 0
    counts, spare = [largest] + [least] * (amount - 1), total - largest - least * (amount - 1)
    while spare > 0:
        candidates = [i for i in range(1, amount) if counts[i] < largest] or [i for i in range(1, amount) if counts[i] < reach]
        mass, left = sum([loads[i] for i in candidates]), spare
        for i in candidates:
            addition = min(reach - counts[i], max(1, left * loads[i] // mass), spare)
            counts[i] = counts[i] + addition
            spare = spare - addition
    return np.array(counts)


def normal_values(key, dims, deviation, limit, cuts=(), held_as=jnp.bfloat16):
    values = jax.random.normal(key, dims, jnp.float32) * deviation
    if len(cuts) > 0:
        values = steps_of(key, dims, cuts, -0.22, 0.18) * values
    return jnp.clip(values, min=-limit, max=limit).astype(held_as)


def setup_inputs(seed: int = 0) -> dict:
    seeds = jax.random.split(jax.random.key(seed), 22)
    resid = draw_resid(jax.random.fold_in(seeds[21], 71), 0)
    queries = draw_queries(jax.random.fold_in(seeds[21], 71), 0)
    new_keys = normal_values(seeds[2], (SEQUENCE_TOTAL, KV_HEADS * HEAD), 1.0, 6.0, ((0, 16), (1, 2)))
    new_values = normal_values(seeds[3], (SEQUENCE_TOTAL, KV_HEADS * HEAD), 3.0, 18.0, ((0, 16), (1, 2)))
    key_cache = draw_key_cache(jax.random.fold_in(seeds[21], 71), 0)
    value_cache = normal_values(seeds[5], (SEQUENCE_TOTAL, KV_HEADS, CACHE_SLOTS, HEAD), 3.0, 18.0, ((0, 16), (1, 2)))
    cum_gate = draw_cum_gate(jax.random.fold_in(seeds[21], 71), 0)
    forget_logit = normal_values(seeds[7], (SEQUENCE_TOTAL, QUERY_HEADS), 1.0, 6.0, ((0, 16), (1, 2)), jnp.float32)
    forget_bias = jnp.clip(-3.0 + 5.0 * jax.random.uniform(seeds[8], (QUERY_HEADS,), jnp.float32) ** steps_of(seeds[8], (QUERY_HEADS,), ((0, 2),), -0.2, 0.2), -3.0, 2.0)
    lengths = touch_ends(jax.random.randint(seeds[9], (SEQUENCE_TOTAL,), CACHE_SLOTS // 8, CACHE_SLOTS + 1), jax.random.fold_in(seeds[9], 1), CACHE_SLOTS // 8, CACHE_SLOTS).astype(jnp.int32)
    out_weight = normal_values(seeds[10], (QUERY_HEADS * HEAD, D), (QUERY_HEADS * HEAD) ** -0.5, 0.1875, ((0, 2),))
    norm_gain = jnp.clip(1.0 + 0.18 * jax.random.normal(seeds[11], (D,), jnp.float32), 0.1, 1.9)
    mix_vector = normal_values(seeds[12], (D,), D ** -0.5, 0.125)
    routes_keys = jax.random.split(jax.random.fold_in(seeds[13], 1), SEQUENCE_TOTAL // SEQ_DEV)
    routes_turns = jax.random.permutation(jax.random.fold_in(seeds[13], 3), SEQUENCE_TOTAL // SEQ_DEV)
    routes = jax.vmap(lambda own, number: shared_out(jax.random.fold_in(seeds[13], 2), own, number, SEQ_DEV, EXPERTS, TOP_K, CAP, 1))(routes_keys, routes_turns).reshape((SEQUENCE_TOTAL, TOP_K))
    route_weight = jnp.clip(0.2 + 0.8 * jax.random.uniform(seeds[14], (SEQUENCE_TOTAL, TOP_K), jnp.float32) ** steps_of(seeds[14], (SEQUENCE_TOTAL, TOP_K), ((0, 16),), -0.2, 0.2), 0.2, 1.0)
    expert_gate = normal_values(seeds[15], (N_EP, D, FF_SPAN), D ** -0.5, 0.125, ((0, 16), (1, 2)))
    expert_up = normal_values(seeds[16], (N_EP, D, FF_SPAN), D ** -0.5, 0.125, ((0, 16), (1, 2)))
    expert_down = normal_values(seeds[17], (N_EP, FF_SPAN, D), FF ** -0.5, 0.109375, ((0, 16), (2, 2)))
    dense_gate = normal_values(seeds[18], (D, FFD), D ** -0.5, 0.125, ((0, 2), (1, 16)))
    dense_up = normal_values(seeds[19], (D, FFD), D ** -0.5, 0.125, ((0, 2), (1, 16)))
    dense_down = normal_values(seeds[20], (FFD, D), FFD ** -0.5, 0.109375, ((0, 16), (1, 2)))
    return dict(resid=resid, queries=queries, new_keys=new_keys, new_values=new_values, key_cache=key_cache, value_cache=value_cache, cum_gate=cum_gate, forget_logit=forget_logit, forget_bias=forget_bias, lengths=lengths, out_weight=out_weight, norm_gain=norm_gain, mix_vector=mix_vector, routes=routes, route_weight=route_weight, expert_gate=expert_gate, expert_up=expert_up, expert_down=expert_down, dense_gate=dense_gate, dense_up=dense_up, dense_down=dense_down)


EPSILON = 1e-06

def slot_table(route_block, expert_ids, capacity):
    blocks = route_block.shape[0]
    flat_routes = route_block.reshape(blocks, 1, -1)
    matched = (flat_routes == expert_ids.reshape(1, -1, 1)).astype(jnp.int32)
    ranking = jnp.cumsum(matched, axis=2) - 1
    slot_ids = jnp.arange(capacity, dtype=jnp.int32)
    taken = (matched[..., None] > 0) & (ranking[..., None] == slot_ids)
    table = jnp.swapaxes(taken, 2, 3).astype(jnp.float32)
    return table.reshape(blocks, expert_ids.shape[0], capacity, route_block.shape[1], route_block.shape[2])

def attend(queries, new_keys, new_values, key_cache, value_cache, cum_gate, forget_logit, forget_bias, lengths):
    seqcount = queries.shape[0]
    kv_local = key_cache.shape[1]
    grouping = QUERY_HEADS // KV_HEADS
    heads_local = kv_local * grouping
    scale_factor = 1.0 / math.sqrt(HEAD)
    query_float = queries.astype(jnp.float32).reshape(seqcount, kv_local, grouping, HEAD)
    scores = jnp.einsum('sgjd,sgpd->sgjp', query_float, key_cache.astype(jnp.float32))
    scores = scores.reshape(seqcount, heads_local, -1) * scale_factor
    own_score = jnp.einsum('sgjd,sgd->sgj', query_float, new_keys.astype(jnp.float32).reshape(seqcount, kv_local, HEAD))
    own_score = own_score.reshape(seqcount, heads_local) * scale_factor
    log_forget = jax.nn.log_sigmoid(forget_logit + forget_bias)
    position = jnp.arange(cum_gate.shape[2], dtype=jnp.int32)
    latest = lax.optimization_barrier(jnp.sum(jnp.where(position == (lengths - 1)[:, None, None], cum_gate, 0.0), axis=2))
    scores = scores + (latest + log_forget)[:, :, None] - cum_gate
    visible = position[None, None, :] < lengths[:, None, None]
    scores = jnp.where(visible, scores, -jnp.inf)
    highest = jnp.maximum(lax.optimization_barrier(jnp.max(scores, axis=2)), own_score)
    weights_past = jnp.exp(scores - highest[:, :, None])
    weight_own = jnp.exp(own_score - highest)
    totals = lax.optimization_barrier(jnp.sum(weights_past, axis=2)) + weight_own
    probs_past = (weights_past / totals[:, :, None]).astype(jnp.bfloat16)
    prob_own = (weight_own / totals).astype(jnp.bfloat16)
    mixed = jnp.einsum('sgjp,sgpd->sgjd', probs_past.astype(jnp.float32).reshape(seqcount, kv_local, grouping, -1), value_cache.astype(jnp.float32))
    mixed = mixed + prob_own.astype(jnp.float32).reshape(seqcount, kv_local, grouping, 1) * new_values.astype(jnp.float32).reshape(seqcount, kv_local, 1, HEAD)
    return mixed.reshape(seqcount, heads_local * HEAD).astype(jnp.bfloat16)

def reference(resid, queries, new_keys, new_values, key_cache, value_cache, cum_gate, forget_logit, forget_bias, lengths, out_weight, norm_gain, mix_vector, routes, route_weight, expert_gate, expert_up, expert_down, dense_gate, dense_up, dense_down):

    def per_block(pieces):
        q_block, k_new, v_new, k_cache, v_cache, gates_block, logit_block, length_block = pieces
        return attend(q_block, k_new, v_new, k_cache, v_cache, gates_block, logit_block, forget_bias, length_block)
    pieces = (queries.reshape(N_EP, SEQ_DEV, -1), new_keys.reshape(N_EP, SEQ_DEV, -1), new_values.reshape(N_EP, SEQ_DEV, -1), key_cache.reshape(N_EP, SEQ_DEV, KV_HEADS, CACHE_SLOTS, HEAD), value_cache.reshape(N_EP, SEQ_DEV, KV_HEADS, CACHE_SLOTS, HEAD), cum_gate.reshape(N_EP, SEQ_DEV, QUERY_HEADS, CACHE_SLOTS), forget_logit.reshape(N_EP, SEQ_DEV, QUERY_HEADS), lengths.reshape(N_EP, SEQ_DEV))
    attended = lax.map(per_block, pieces).reshape(SEQUENCE_TOTAL, QUERY_HEADS * HEAD)
    projected = jnp.dot(attended, out_weight, preferred_element_type=jnp.float32).astype(jnp.bfloat16)
    state = resid.astype(jnp.float32) + projected.astype(jnp.float32)
    inverse = lax.rsqrt(lax.optimization_barrier(jnp.mean(state * state, axis=1)) + EPSILON)
    normed = (state * inverse[:, None] * norm_gain).astype(jnp.bfloat16)
    gate = jax.nn.sigmoid(inverse * lax.optimization_barrier(jnp.sum(state * norm_gain * mix_vector.astype(jnp.float32), axis=1)))
    dense_g = jnp.dot(normed, dense_gate, preferred_element_type=jnp.float32)
    dense_u = jnp.dot(normed, dense_up, preferred_element_type=jnp.float32)
    dense_hidden = (jax.nn.silu(dense_g) * dense_u).astype(jnp.bfloat16)
    dense = jnp.dot(dense_hidden, dense_down, preferred_element_type=jnp.float32)
    route_block = routes.reshape(N_EP, SEQ_DEV, TOP_K)
    weight_block = route_weight.reshape(N_EP, SEQ_DEV, TOP_K)
    normed_block = normed.reshape(N_EP, SEQ_DEV, D).astype(jnp.float32)
    gate_blocks = expert_gate.reshape(EXPERTS, EXP_SPAN, D, FF_SPAN)
    up_blocks = expert_up.reshape(EXPERTS, EXP_SPAN, D, FF_SPAN)
    down_blocks = expert_down.reshape(EXPERTS, EXP_SPAN, FF_SPAN, D)

    def expert_step(total, inputs):
        expert_id, gate_part, up_part, down_part = inputs
        w_gate = jnp.transpose(gate_part, (1, 0, 2)).reshape(D, FF)
        w_up = jnp.transpose(up_part, (1, 0, 2)).reshape(D, FF)
        w_down = down_part.reshape(FF, D)
        table = slot_table(route_block, expert_id.reshape(1), CAP)[:, 0]
        picked = lax.optimization_barrier(jnp.sum(table, axis=3))
        chosen = jnp.einsum('bct,btd->bcd', picked, normed_block).astype(jnp.bfloat16).reshape(N_EP * CAP, D)
        gated = jnp.dot(chosen, w_gate, preferred_element_type=jnp.float32)
        upped = jnp.dot(chosen, w_up, preferred_element_type=jnp.float32)
        hidden = (jax.nn.silu(gated) * upped).astype(jnp.bfloat16)
        outputs = jnp.dot(hidden, w_down, preferred_element_type=jnp.float32).reshape(N_EP, CAP, D)
        share = jnp.einsum('bctk,btk,bcd->btd', table, weight_block, outputs, precision=lax.Precision.HIGHEST)
        return (total + share.reshape(SEQUENCE_TOTAL, D), None)
    routed, unused = lax.scan(expert_step, jnp.zeros((SEQUENCE_TOTAL, D), jnp.float32), (jnp.arange(EXPERTS, dtype=jnp.int32), gate_blocks, up_blocks, down_blocks))
    result = state + routed + gate[:, None] * dense
    return result.astype(jnp.bfloat16)
```

```python
import math

import jax
import jax.numpy as jnp
from jax import lax
from jax.sharding import PartitionSpec as P

QUERY_HEADS = 8
KV_HEADS = 4
HEAD = 128
TOP_K = 2
EXP_SPAN = 4


EPSILON = 1e-06


def slot_table(route_block, expert_ids, capacity):
    blocks = route_block.shape[0]
    flat_routes = route_block.reshape(blocks, 1, -1)
    matched = (flat_routes == expert_ids.reshape(1, -1, 1)).astype(jnp.int32)
    ranking = jnp.cumsum(matched, axis=2) - 1
    slot_ids = jnp.arange(capacity, dtype=jnp.int32)
    taken = (matched[..., None] > 0) & (ranking[..., None] == slot_ids)
    table = jnp.swapaxes(taken, 2, 3).astype(jnp.float32)
    return table.reshape(
        blocks, expert_ids.shape[0], capacity, route_block.shape[1], route_block.shape[2]
    )


def attend(
    queries,
    new_keys,
    new_values,
    key_cache,
    value_cache,
    cum_gate,
    forget_logit,
    forget_bias,
    lengths,
):
    seqcount = queries.shape[0]
    kv_local = key_cache.shape[1]
    grouping = QUERY_HEADS // KV_HEADS
    heads_local = kv_local * grouping
    scale_factor = 1.0 / math.sqrt(HEAD)
    query_float = queries.astype(jnp.float32).reshape(seqcount, kv_local, grouping, HEAD)
    scores = jnp.einsum("sgjd,sgpd->sgjp", query_float, key_cache.astype(jnp.float32))
    scores = scores.reshape(seqcount, heads_local, -1) * scale_factor
    own_score = jnp.einsum(
        "sgjd,sgd->sgj", query_float, new_keys.astype(jnp.float32).reshape(seqcount, kv_local, HEAD)
    )
    own_score = own_score.reshape(seqcount, heads_local) * scale_factor
    log_forget = jax.nn.log_sigmoid(forget_logit + forget_bias)
    position = jnp.arange(cum_gate.shape[2], dtype=jnp.int32)
    latest = jnp.sum(jnp.where(position == (lengths - 1)[:, None, None], cum_gate, 0.0), axis=2)
    scores = scores + (latest + log_forget)[:, :, None] - cum_gate
    visible = position[None, None, :] < lengths[:, None, None]
    scores = jnp.where(visible, scores, -jnp.inf)
    highest = jnp.maximum(jnp.max(scores, axis=2), own_score)
    weights_past = jnp.exp(scores - highest[:, :, None])
    weight_own = jnp.exp(own_score - highest)
    totals = jnp.sum(weights_past, axis=2) + weight_own
    probs_past = (weights_past / totals[:, :, None]).astype(jnp.bfloat16)
    prob_own = (weight_own / totals).astype(jnp.bfloat16)
    mixed = jnp.einsum(
        "sgjp,sgpd->sgjd",
        probs_past.astype(jnp.float32).reshape(seqcount, kv_local, grouping, -1),
        value_cache.astype(jnp.float32),
    )
    mixed = mixed + prob_own.astype(jnp.float32).reshape(
        seqcount, kv_local, grouping, 1
    ) * new_values.astype(jnp.float32).reshape(seqcount, kv_local, 1, HEAD)
    return mixed.reshape(seqcount, heads_local * HEAD).astype(jnp.bfloat16)


def slot_body(
    resid,
    queries,
    new_keys,
    new_values,
    key_cache,
    value_cache,
    cum_gate,
    forget_logit,
    forget_bias,
    lengths,
    out_weight,
    norm_gain,
    mix_vector,
    routes,
    route_weight,
    expert_gate,
    expert_up,
    expert_down,
    dense_gate,
    dense_up,
    dense_down,
):
    attended = attend(
        queries,
        new_keys,
        new_values,
        key_cache,
        value_cache,
        cum_gate,
        forget_logit,
        forget_bias,
        lengths,
    )
    head_part = jnp.dot(attended, out_weight, preferred_element_type=jnp.float32)
    projected = lax.psum(head_part.astype(jnp.bfloat16), "tp")
    state_full = resid.astype(jnp.float32) + projected.astype(jnp.float32)
    inverse = lax.rsqrt(jnp.mean(state_full * state_full, axis=1) + EPSILON)
    scaled_full = state_full * norm_gain
    gate = jax.nn.sigmoid(inverse * jnp.sum(scaled_full * mix_vector.astype(jnp.float32), axis=1))
    channel_width = resid.shape[1] // lax.axis_size("tp")
    offset = lax.axis_index("tp") * channel_width
    state = lax.dynamic_slice_in_dim(state_full, offset, channel_width, 1)
    normed = (
        lax.dynamic_slice_in_dim(scaled_full, offset, channel_width, 1) * inverse[:, None]
    ).astype(jnp.bfloat16)
    ep_count = lax.axis_size("ep")
    tokens = resid.shape[0]
    experts = ep_count // EXP_SPAN
    capacity = min(tokens, 2 * ((tokens * TOP_K + experts - 1) // experts))
    w_gate = expert_gate[0]
    w_up = expert_up[0]
    w_down = expert_down[0]
    table = slot_table(
        routes.reshape(1, tokens, TOP_K), jnp.arange(experts, dtype=jnp.int32), capacity
    )[0]
    picked = jnp.sum(table, axis=3).astype(jnp.bfloat16)
    outgoing = jnp.einsum("ect,td->ecd", picked, normed, preferred_element_type=jnp.float32).astype(
        jnp.bfloat16
    )
    outgoing = jnp.repeat(outgoing, EXP_SPAN, axis=0)
    arrived = lax.all_to_all(outgoing, "ep", split_axis=0, concat_axis=0, tiled=True)
    flat_rows = arrived.reshape(-1, arrived.shape[2])
    gated = lax.psum(
        jnp.dot(flat_rows, w_gate, preferred_element_type=jnp.float32).astype(jnp.bfloat16), "tp"
    ).astype(jnp.float32)
    upped = lax.psum(
        jnp.dot(flat_rows, w_up, preferred_element_type=jnp.float32).astype(jnp.bfloat16), "tp"
    ).astype(jnp.float32)
    hidden = (jax.nn.silu(gated) * upped).astype(jnp.bfloat16)
    produced = jnp.dot(hidden, w_down, preferred_element_type=jnp.float32)
    produced = produced.reshape(arrived.shape[0], arrived.shape[1], -1)
    returned = lax.all_to_all(
        produced.astype(jnp.bfloat16), "ep", split_axis=0, concat_axis=0, tiled=True
    ).astype(produced.dtype)
    outputs = returned.reshape(experts, EXP_SPAN, capacity, -1).sum(axis=1)
    routed = jnp.einsum(
        "ectk,tk,ecd->td", table, route_weight, outputs, precision=lax.Precision.HIGHEST
    )
    piece = lax.all_gather(normed, "ep", axis=0, tiled=True)
    paired = jnp.concatenate(
        [
            jnp.dot(piece, dense_gate, preferred_element_type=jnp.float32),
            jnp.dot(piece, dense_up, preferred_element_type=jnp.float32),
        ],
        axis=1,
    )
    paired = lax.psum(paired.astype(jnp.bfloat16), "tp").astype(jnp.float32)
    hidden_width = dense_gate.shape[1]
    dense_hidden = (jax.nn.silu(paired[:, :hidden_width]) * paired[:, hidden_width:]).astype(
        jnp.bfloat16
    )
    dense = lax.psum_scatter(
        jnp.dot(dense_hidden, dense_down, preferred_element_type=jnp.float32),
        "ep",
        scatter_dimension=0,
        tiled=True,
    )
    result = state + routed + gate[:, None] * dense
    return result.astype(jnp.bfloat16)


def exchange(rows, axis, distance):
    count = lax.axis_size(axis)
    return lax.ppermute(rows, axis, [(i, i ^ distance) for i in range(count)])


def rows_body(
    resid,
    queries,
    new_keys,
    new_values,
    key_cache,
    value_cache,
    cum_gate,
    forget_logit,
    forget_bias,
    lengths,
    out_weight,
    norm_gain,
    mix_vector,
    routes,
    route_weight,
    expert_gate,
    expert_up,
    expert_down,
    dense_gate,
    dense_up,
    dense_down,
):
    ep_count = lax.axis_size("ep")
    tokens, width = resid.shape
    experts = ep_count // EXP_SPAN
    channel_width = width // 2
    side = lax.axis_index("tp")
    attended = attend(
        queries,
        new_keys,
        new_values,
        key_cache,
        value_cache,
        cum_gate,
        forget_logit,
        forget_bias,
        lengths,
    )
    head_part = jnp.dot(attended, out_weight, preferred_element_type=jnp.float32)
    head_part = head_part.astype(jnp.bfloat16)
    other_part = exchange(head_part, "tp", 1)
    projected = head_part.astype(jnp.float32) + other_part.astype(jnp.float32)
    projected = projected.astype(jnp.bfloat16)
    state_full = resid.astype(jnp.float32) + projected.astype(jnp.float32)
    inverse = lax.rsqrt(jnp.mean(state_full * state_full, axis=1) + EPSILON)
    scaled_full = state_full * norm_gain
    gate = jax.nn.sigmoid(inverse * jnp.sum(scaled_full * mix_vector.astype(jnp.float32), axis=1))
    offset = side * channel_width
    state = lax.dynamic_slice_in_dim(state_full, offset, channel_width, 1)
    normed = (
        lax.dynamic_slice_in_dim(scaled_full, offset, channel_width, 1) * inverse[:, None]
    ).astype(jnp.bfloat16)
    chosen = routes[:, :, None] == jnp.arange(experts, dtype=jnp.int32)
    shares = jnp.sum(jnp.where(chosen, route_weight[:, :, None], 0.0), axis=1)
    shares = jnp.concatenate([gate[:, None], shares], axis=1)
    high = shares.astype(jnp.bfloat16)
    low = (shares - high.astype(jnp.float32)).astype(jnp.bfloat16)
    filler = (-2 * shares.shape[1]) % 128
    payload = jnp.concatenate(
        [normed, high, low, jnp.zeros((tokens, filler), jnp.bfloat16)], axis=1
    )
    own_expert = lax.axis_index("ep") // EXP_SPAN
    columns = 1 + experts

    w_gate, w_up, w_down = expert_gate[0], expert_up[0], expert_down[0]

    def partials(rows):
        x = rows[:, :channel_width]
        parts = [
            jnp.dot(x, w, preferred_element_type=jnp.float32)
            for w in (w_gate, w_up, dense_gate, dense_up)
        ]
        joined = jnp.concatenate(parts, axis=1)
        half = rows.shape[0] // 2
        mine = lax.dynamic_slice_in_dim(joined, side * half, half, 0)
        theirs = lax.dynamic_slice_in_dim(joined, (1 - side) * half, half, 0)
        extra = rows[:, channel_width:].astype(jnp.float32)
        weights = extra[:, :columns] + extra[:, columns : 2 * columns]
        weights = lax.dynamic_slice_in_dim(weights, side * half, half, 0)
        return mine, theirs.astype(jnp.bfloat16), weights

    span = w_gate.shape[1]
    dense_span = dense_gate.shape[1]

    def hidden_rows(mine, arrived, weights):
        total = mine + arrived.astype(jnp.float32)
        gated, upped = total[:, :span], total[:, span : 2 * span]
        d_gated = total[:, 2 * span : 2 * span + dense_span]
        d_upped = total[:, 2 * span + dense_span :]
        share = lax.dynamic_slice_in_dim(weights, 1 + own_expert, 1, 1)
        hidden = jax.nn.silu(gated) * upped * share
        d_hidden = jax.nn.silu(d_gated) * d_upped * weights[:, :1]
        return jnp.concatenate([hidden, d_hidden], axis=1).astype(jnp.bfloat16)

    def downward(mine, arrived):
        first = jnp.where(side == 0, mine, arrived)
        second = jnp.where(side == 0, arrived, mine)
        hidden = jnp.concatenate([first, second], axis=0)
        out = jnp.dot(hidden[:, :span], w_down, preferred_element_type=jnp.float32)
        return out + jnp.dot(hidden[:, span:], dense_down, preferred_element_type=jnp.float32)

    pair = jnp.concatenate([payload, exchange(payload, "ep", 2)], axis=0)
    near = jnp.concatenate([pair, exchange(pair, "ep", 1)], axis=0)
    groups = ep_count // 4
    far_pairs = jnp.concatenate([exchange(pair, "ep", 4 * k) for k in range(1, groups)], axis=0)
    far = jnp.concatenate([far_pairs, exchange(far_pairs, "ep", 1)], axis=0)

    mine_n, theirs_n, weights_n = partials(near)
    sums_n = exchange(theirs_n, "tp", 1)
    mine_f, theirs_f, weights_f = partials(far)
    sums_f = exchange(theirs_f, "tp", 1)
    hidden_n = hidden_rows(mine_n, sums_n, weights_n)
    rows_n = exchange(hidden_n, "tp", 1)
    hidden_f = hidden_rows(mine_f, sums_f, weights_f)
    rows_f = exchange(hidden_f, "tp", 1)
    out_n = downward(hidden_n, rows_n)
    out_f = downward(hidden_f, rows_f)

    def fold(kept, sent, distance):
        return kept + exchange(sent.astype(jnp.bfloat16), "ep", distance).astype(jnp.float32)

    half_n = out_n.shape[0] // 2
    own_n = fold(out_n[:half_n], out_n[half_n:], 1)
    half_f = out_f.shape[0] // 2
    own_f = fold(out_f[:half_f], out_f[half_f:], 1).reshape(groups - 1, 2, tokens, -1)
    total = fold(own_n[:tokens], own_n[tokens:], 2)
    chip_f = fold(own_f[:, 0], own_f[:, 1], 2)
    for k in range(1, groups):
        total = fold(total, chip_f[k - 1], 4 * k)
    return (state + total).astype(jnp.bfloat16)


def body(*arrays):
    ep_count = lax.axis_size("ep")
    tokens = arrays[0].shape[0]
    experts = ep_count // EXP_SPAN
    capacity = min(tokens, 2 * ((tokens * TOP_K + experts - 1) // experts))
    powers = ep_count >= 8 and ep_count & (ep_count - 1) == 0
    if capacity == tokens and powers and lax.axis_size("tp") == 2:
        return rows_body(*arrays)
    return slot_body(*arrays)


def solution(mesh):
    placed = (
        P("ep", None),
        P("ep", "tp"),
        P("ep", "tp"),
        P("ep", "tp"),
        P("ep", "tp", None, None),
        P("ep", "tp", None, None),
        P("ep", "tp", None),
        P("ep", "tp"),
        P("tp"),
        P("ep"),
        P("tp", None),
        P(),
        P(),
        P("ep", None),
        P("ep", None),
        P("ep", "tp", None),
        P("ep", "tp", None),
        P("ep", None, "tp"),
        P("tp", "ep"),
        P("tp", "ep"),
        P("ep", "tp"),
    )
    return jax.shard_map(body, mesh=mesh, in_specs=placed, out_specs=P("ep", "tp"), check_vma=False)
```
